32 devices in a mesh: rep: 2 (over y), fs: 4 (over z), tp: 4 (over x, core).
Axes of the slice: x: 2, y: 2, z: 4, core: 2. Of those that a mesh axis runs over, the one named last changes fastest.
Arguments:
- tokens: bfloat16 [2048, 2048], P(('rep', 'fs')), may hold values from -6 to 6
- norm_gains: float32 [3, 2048], replicated, may hold values from 0.1 to 1.9
- gate_weight: float32 [2048, 3072], P('fs', 'tp'), may hold values from -0.125 to 0.125
- up_weight: float32 [2048, 3072], P('fs', 'tp'), may hold values from -0.125 to 0.125
- hidden_scales: float32 [2, 3072], P(None, 'tp'), may hold values from 0.5 to 2
- down_weight: float32 [3072, 2048], P('tp', 'fs'), may hold values from -0.21875 to 0.21875
- down_scale: float32 [2048], P('fs'), may hold values from 0.5 to 2
- mix_in: float32 [2048, 512], P('fs'), may hold values from -0.125 to 0.125
- in_scale: float32 [512], replicated, may hold values from 0.5 to 2
- pool_map: float32 [4, 128, 128], replicated, may hold values from -0.5 to 0.5
- pool_scale: float32 [512], P('tp'), may hold values from 0.5 to 2
- mix_out: float32 [512, 2048], P('tp', 'fs'), may hold values from -0.25 to 0.25
- out_scale: float32 [2048], P('fs'), may hold values from 0.5 to 2
Outputs:
- layer_out: bfloat16 [2048, 2048], P(('rep', 'fs'))
The draws below stay inside these ranges and needn't reach their ends.
All inputs are finite; a program needn't handle non-finite values.
Results may differ from the reference program's by a relative error of at most 0.02.
Values may be sent and summed in bfloat16 or wider, within the bound.
A program may use at most 64 MiB of HBM per device.

```python
import math
import jax
import jax.numpy as jnp
from jax import lax

D = 2048
FF = 3072
DP = 512
GROUPS = 4
GC = 128
TOK = 256
TOKENS = 2048
N_TP = 4


def steps_of(key, shape, pieces, least, largest):
    factor_of, own = 1.0, jax.random.fold_in(key, 6)
    for axis_at, shards_of in pieces:
        heights = jnp.exp(jax.random.uniform(jax.random.fold_in(own, axis_at), (shards_of,), jnp.float32, least / len(pieces), largest / len(pieces)))
        factor_of = factor_of * jnp.repeat(heights, shape[axis_at] // shards_of).reshape([-1 if axis == axis_at else 1 for axis in range(len(shape))])
    return factor_of


def centred(key, shape, spread, bound, cuts=(), kind=jnp.bfloat16):
    entries = jax.random.normal(key, shape, jnp.float32) * spread
    if len(cuts) > 0:
        entries = steps_of(key, shape, cuts, -0.22, 0.18) * entries
    return jnp.clip(entries, min=-bound, max=bound).astype(kind)


def setup_inputs(seed: int = 0) -> dict:
    keys = jax.random.split(jax.random.key(seed), 14)
    tokens = centred(keys[0], (TOKENS, D), 1.0, 6.0, ((0, 8),))
    norm_gains = jnp.clip(1.0 + 0.18 * jax.random.normal(keys[1], (3, D), jnp.float32), 0.1, 1.9)
    gate_weight = centred(keys[2], (D, FF), D ** -0.5, 0.125, ((0, 4), (1, 4)), jnp.float32)
    up_weight = centred(keys[3], (D, FF), D ** -0.5, 0.125, ((0, 4), (1, 4)), jnp.float32)
    hidden_scales = jnp.clip(jnp.exp(math.log(2.0) - 1.3862944 * jax.random.uniform(keys[4], (2, FF), jnp.float32) ** steps_of(keys[4], (2, FF), ((1, 4),), -0.2, 0.2)), 0.5, 2.0)
    down_weight = centred(keys[5], (FF, D), (FF // 4) ** -0.5, 0.21875, ((0, 4), (1, 4)), jnp.float32)
    down_scale = jnp.clip(jnp.exp(math.log(2.0) - 1.3862944 * jax.random.uniform(keys[6], (D,), jnp.float32) ** steps_of(keys[6], (D,), ((0, 4),), -0.2, 0.2)), 0.5, 2.0)
    mix_in = centred(keys[7], (D, DP), D ** -0.5, 0.125, ((0, 4),), jnp.float32)
    in_scale = jnp.clip(jnp.exp(jax.random.uniform(keys[8], (DP,), jnp.float32, math.log(0.5), math.log(2.0))), 0.5, 2.0)
    pool_map = centred(keys[9], (GROUPS, GC, GC), GC ** -0.5, 0.5, (), jnp.float32)
    pool_scale = jnp.clip(jnp.exp(math.log(2.0) - 1.3862944 * jax.random.uniform(keys[10], (DP,), jnp.float32) ** steps_of(keys[10], (DP,), ((0, 4),), -0.2, 0.2)), 0.5, 2.0)
    mix_out = centred(keys[11], (DP, D), DP ** -0.5, 0.25, ((0, 4), (1, 4)), jnp.float32)
    out_scale = jnp.clip(jnp.exp(math.log(2.0) - 1.3862944 * jax.random.uniform(keys[12], (D,), jnp.float32) ** steps_of(keys[12], (D,), ((0, 4),), -0.2, 0.2)), 0.5, 2.0)
    return {"tokens": tokens, "norm_gains": norm_gains, "gate_weight": gate_weight, "up_weight": up_weight, "hidden_scales": hidden_scales, "down_weight": down_weight, "down_scale": down_scale, "mix_in": mix_in, "in_scale": in_scale, "pool_map": pool_map, "pool_scale": pool_scale, "mix_out": mix_out, "out_scale": out_scale}


eps = 1e-06
widest = 16

def normed(values, gain):
    mean_sq = lax.optimization_barrier(jnp.mean(values * values, axis=-1, keepdims=True))
    return (values * lax.rsqrt(mean_sq + eps) * gain).astype(jnp.bfloat16)

def feed_forward(hidden_in, gate_bf, up_bf, down_bf, hidden_scales, down_scale):
    gate = jnp.dot(hidden_in, gate_bf, preferred_element_type=jnp.float32) * hidden_scales[0]
    upper = jnp.dot(hidden_in, up_bf, preferred_element_type=jnp.float32) * hidden_scales[1]
    hidden = (jax.nn.silu(gate) * upper).astype(jnp.bfloat16)
    block_ff = FF // N_TP
    total = jnp.zeros((hidden_in.shape[0], D), jnp.float32)
    for block_index in range(N_TP):
        lower = block_index * block_ff
        part = jnp.dot(hidden[:, lower:lower + block_ff], down_bf[lower:lower + block_ff], preferred_element_type=jnp.float32)
        total = total + part.astype(jnp.bfloat16).astype(jnp.float32)
    return total * down_scale

def pool_rows(pool_in):
    values = pool_in.astype(jnp.float32)
    length = values.shape[1]
    channel = jnp.arange(DP, dtype=jnp.int32)
    window = jnp.left_shift(jnp.int32(2), channel // GC)
    position = jnp.arange(length, dtype=jnp.int32)[:, None]
    summed = jnp.zeros_like(values)
    for offset in range(widest):
        shifted = jnp.pad(values, ((0, 0), (offset, 0), (0, 0)))[:, :length]
        summed = summed + jnp.where(offset < window, shifted, 0.0)
    counts = jnp.minimum(position + 1, window).astype(jnp.float32)
    return (summed / counts - values).astype(jnp.bfloat16)

def reference(tokens, norm_gains, gate_weight, up_weight, hidden_scales, down_weight, down_scale, mix_in, in_scale, pool_map, pool_scale, mix_out, out_scale):
    gate_bf = gate_weight.astype(jnp.bfloat16)
    up_bf = up_weight.astype(jnp.bfloat16)
    down_bf = down_weight.astype(jnp.bfloat16)
    resid = tokens.astype(jnp.float32)
    first = normed(resid, norm_gains[0])
    resid_one = resid + 0.5 * feed_forward(first, gate_bf, up_bf, down_bf, hidden_scales, down_scale)
    second = normed(resid_one, norm_gains[1])
    pool_in = (jnp.dot(second, mix_in.astype(jnp.bfloat16), preferred_element_type=jnp.float32) * in_scale).astype(jnp.bfloat16)
    pooled = pool_rows(pool_in.reshape(-1, TOK, DP)).reshape(-1, GROUPS, GC)
    map_bf = pool_map.astype(jnp.bfloat16)
    grouped = jnp.einsum('rgc,gcd->rgd', pooled.astype(jnp.float32), map_bf.astype(jnp.float32))
    pool_out = (grouped.reshape(-1, DP) * pool_scale).astype(jnp.bfloat16)
    out_bf = mix_out.astype(jnp.bfloat16)
    block_dp = DP // N_TP
    mixed = jnp.zeros_like(resid)
    for block_index in range(N_TP):
        lower = block_index * block_dp
        part = jnp.dot(pool_out[:, lower:lower + block_dp], out_bf[lower:lower + block_dp], preferred_element_type=jnp.float32)
        mixed = mixed + part.astype(jnp.bfloat16).astype(jnp.float32)
    resid_two = resid_one + mixed * out_scale
    third = normed(resid_two, norm_gains[2])
    final = resid_two + 0.5 * feed_forward(third, gate_bf, up_bf, down_bf, hidden_scales, down_scale)
    return final.astype(jnp.bfloat16)
```

```python
import functools

import jax
import jax.numpy as jnp
from jax import lax
from jax.experimental import pallas as pl
from jax.experimental.pallas import tpu as pltpu
from jax.sharding import PartitionSpec as P

eps = 1e-06
widest = 16


def normed(values, gain):
    mean_sq = jnp.mean(values * values, axis=-1, keepdims=True)
    return (values * lax.rsqrt(mean_sq + eps) * gain).astype(jnp.bfloat16)


def scatter_rows(term_fn, share):
    return lax.psum_scatter(
        term_fn(jnp.int32(0), lax.axis_size("tp") * share).astype(jnp.bfloat16),
        "tp",
        scatter_dimension=0,
        tiled=True,
    ).astype(jnp.float32)


def whole_rows(values):
    return lax.all_gather(values, "tp", axis=0, tiled=True)


def fetch_mixer(in_cols, mix_out):
    return (
        lax.all_gather(in_cols.astype(jnp.bfloat16), "fs", axis=0, tiled=True),
        lax.all_gather(mix_out.astype(jnp.bfloat16), "fs", axis=1, tiled=True),
    )


def hidden_units(rows_in, gate_full, up_full, hidden_scales):
    gate = jnp.dot(rows_in, gate_full, preferred_element_type=jnp.float32) * hidden_scales[0]
    upper = jnp.dot(rows_in, up_full, preferred_element_type=jnp.float32) * hidden_scales[1]
    return (jax.nn.silu(gate) * upper).astype(jnp.bfloat16)


def ffn_partial(normed_rows, gate_full, up_full, down_full, hidden_scales, share):

    def term_rows(row_start, row_count):
        hidden = hidden_units(normed_rows, gate_full, up_full, hidden_scales)
        return jnp.dot(hidden, down_full, preferred_element_type=jnp.float32)

    return scatter_rows(term_rows, share)


def per_device(
    tokens,
    norm_gains,
    gate_weight,
    up_weight,
    hidden_scales,
    down_weight,
    down_scale,
    mix_in,
    in_scale,
    pool_map,
    pool_scale,
    mix_out,
    out_scale,
):
    tp_width = lax.axis_size("tp")
    tp_rank = lax.axis_index("tp")
    seq_rows = tokens.shape[0]
    share = seq_rows // tp_width
    local_channels = mix_out.shape[0]
    group_width = pool_map.shape[1]
    needed = max(group_width, local_channels)
    first_channel = tp_rank * local_channels
    in_start = first_channel // group_width * group_width
    in_cols = lax.dynamic_slice_in_dim(mix_in, in_start, needed, 1)
    scale_cols = lax.dynamic_slice_in_dim(in_scale, in_start, needed, 0)
    down_cols, out_cols = (
        lax.all_gather(down_scale, "fs", axis=0, tiled=True),
        lax.all_gather(out_scale, "fs", axis=0, tiled=True),
    )
    gate_bf = gate_weight.astype(jnp.bfloat16)
    up_bf = up_weight.astype(jnp.bfloat16)
    down_bf = down_weight.astype(jnp.bfloat16)
    resid_all = tokens.astype(jnp.float32)
    first = normed(resid_all, norm_gains[0])
    gate_full, up_full, down_full = (
        lax.all_gather(gate_bf, "fs", axis=0, tiled=True),
        lax.all_gather(up_bf, "fs", axis=0, tiled=True),
        lax.all_gather(down_bf, "fs", axis=1, tiled=True),
    )
    ffn_one = ffn_partial(first, gate_full, up_full, down_full, hidden_scales, share)
    own_rows = lax.dynamic_slice_in_dim(resid_all, tp_rank * share, share, 0)
    resid_one = own_rows + 0.5 * (ffn_one * down_cols)
    second = whole_rows(normed(resid_one, norm_gains[1]))
    in_full, out_full = fetch_mixer(in_cols, mix_out)
    pool_in = (jnp.dot(second, in_full, preferred_element_type=jnp.float32) * scale_cols).astype(
        jnp.bfloat16
    )
    channel = in_start + jnp.arange(needed, dtype=jnp.int32)
    window = jnp.left_shift(jnp.int32(2), channel // group_width)
    position = jnp.arange(seq_rows, dtype=jnp.int32)[:, None]
    values = pool_in.astype(jnp.float32)
    summed = jnp.zeros_like(values)
    for offset in range(widest):
        shifted = jnp.pad(values, ((offset, 0), (0, 0)))[:seq_rows]
        summed = summed + jnp.where(offset < window, shifted, 0.0)
    counts = jnp.minimum(position + 1, window).astype(jnp.float32)
    pooled = (summed / counts - values).astype(jnp.bfloat16)
    map_bf = pool_map.astype(jnp.bfloat16)
    if local_channels < group_width:
        group_index = first_channel // group_width
        column_start = first_channel % group_width
        map_cols = lax.dynamic_slice(
            map_bf, (group_index, jnp.int32(0), column_start), (1, group_width, local_channels)
        )[0]
        grouped = jnp.dot(pooled, map_cols, preferred_element_type=jnp.float32)
    else:
        held_groups = local_channels // group_width
        maps_held = lax.dynamic_slice_in_dim(map_bf, first_channel // group_width, held_groups, 0)
        grouped = jnp.einsum(
            "tgc,gcd->tgd",
            pooled.reshape(seq_rows, held_groups, group_width),
            maps_held,
            preferred_element_type=jnp.float32,
        ).reshape(seq_rows, local_channels)
    pool_out = (grouped * pool_scale).astype(jnp.bfloat16)

    def mixer_rows(row_start, row_count):
        return jnp.dot(pool_out, out_full, preferred_element_type=jnp.float32)

    mixed = scatter_rows(mixer_rows, share)
    resid_two = resid_one + mixed * out_cols
    third = whole_rows(normed(resid_two, norm_gains[2]))
    ffn_two = ffn_partial(third, gate_full, up_full, down_full, hidden_scales, share)
    final_rows = (resid_two + 0.5 * (ffn_two * down_cols)).astype(jnp.bfloat16)
    return whole_rows(final_rows)


MESH = pl.DeviceIdType.MESH
QUARTERS = 4
TILE = 256
bf16 = jnp.bfloat16
f32 = jnp.float32


def fits_kernel(mesh):
    return mesh.shape["rep"] == 2 and mesh.shape["fs"] == 4 and mesh.shape["tp"] == 4


def layer_kernel(
    n, tok, gains, gu_in, hs, dn_in, wi_in, wo_in, isc, pmap, ps_in, sc_in,
    out, gu_buf, dn_buf, wi_all, wo_all, sc_all, ps_all,
    first, gacc, hidden, stage, rs, r1, second, pool, r2, third, rs_a, s_b, rs_b,
    ring_send, ring_recv, sc_send, sc_recv, tp_send, tp_recv, rs_send, rs_recv, ag_send, ag_recv, loc,
):
    rep, fs, me = lax.axis_index("rep"), lax.axis_index("fs"), lax.axis_index("tp")
    width = tok.shape[1]
    seq = tok.shape[0]
    slab = width // n
    share = seq // 4
    halo = widest
    units = hs.shape[1]
    gc = pmap.shape[1]
    core = me % 2
    mate = me + 1 - 2 * core
    across = (me + 2) % 4
    diag = (mate + 2) % 4
    peers = {1: mate, 2: across, 3: diag}

    def owner_cols(d):
        return pl.ds(pl.multiple_of(((fs + d) % n) * slab, slab), slab)

    def to_fs(offset):
        return {"fs": (fs + offset + n) % n}

    barrier = pltpu.get_barrier_semaphore()
    for offset in range(1, n):
        pl.semaphore_signal(barrier, inc=1, device_id=to_fs(offset), device_id_type=MESH)
    for k in (1, 2, 3):
        pl.semaphore_signal(barrier, inc=1, device_id={"tp": peers[k]}, device_id_type=MESH)
    pl.semaphore_signal(barrier, inc=1, device_id={"rep": 1 - rep}, device_id_type=MESH)
    pl.semaphore_wait(barrier, n - 1 + 4)

    WI, WO, GU, DN = range(4)

    def slot(t, d):
        if t == WI:
            return wi_in if d == 0 else wi_all.at[0, d]
        if t == WO:
            return wo_in if d == 0 else wo_all.at[0, d]
        if t == GU:
            return gu_in if d == 0 else gu_buf.at[d - 1]
        return dn_in if d == 0 else dn_buf.at[d - 1]

    def piece(t, d, q):
        ref = slot(t, d)
        rows = ref.shape[0] // QUARTERS
        at = q + rep * (QUARTERS - 1 - 2 * q)
        return ref.at[pl.ds(pl.multiple_of(at * rows, rows), rows), :]

    def via(d, q):
        if d == n // 2:
            return (1, -1, 0, 0)[q]
        if q == QUARTERS - 1:
            return 0
        return 1 if d < n // 2 else -1

    started = []

    def ring_copy(t, d, q):
        way = via(d, q)
        if way == 0:
            src, dev = piece(t, d, QUARTERS - 1 - q), {"rep": 1 - rep}
            dst = piece(t, d, QUARTERS - 1 - q)
        else:
            src, dev = piece(t, (d - way) % n, q), to_fs(-way)
            dst = piece(t, d, q)
        return pltpu.make_async_remote_copy(
            src_ref=src, dst_ref=dst, send_sem=ring_send.at[t, d - 1, q], recv_sem=ring_recv.at[t, d - 1, q],
            device_id=dev, device_id_type=MESH,
        )

    def send(t, d, q):
        copy = ring_copy(t, d, q)
        copy.start()
        started.append(copy)

    def arrived(t, d, q):
        here = piece(t, d, q)
        pltpu.make_async_remote_copy(
            src_ref=here, dst_ref=here, send_sem=ring_send.at[t, d - 1, q], recv_sem=ring_recv.at[t, d - 1, q],
            device_id=to_fs(1), device_id_type=MESH,
        ).wait_recv()

    def remote(src, dst, s_sem, r_sem, dev):
        copy = pltpu.make_async_remote_copy(
            src_ref=src, dst_ref=dst, send_sem=s_sem, recv_sem=r_sem, device_id=dev, device_id_type=MESH
        )
        copy.start()
        started.append(copy)
        return copy

    def landed(dst, s_sem, r_sem):
        pltpu.make_async_remote_copy(
            src_ref=dst, dst_ref=dst, send_sem=s_sem, recv_sem=r_sem, device_id={"tp": mate}, device_id_type=MESH
        ).wait_recv()

    def send_own(t):
        for q in range(QUARTERS - 1):
            send(t, 1, q)
            send(t, n - 1, q)

    def relay_near(t):
        arrived(t, 1, 0)
        send(t, 2, 0)
        send(t, 1, 3)
        arrived(t, n - 1, 0)
        send(t, n - 1, 3)
        arrived(t, n - 1, 1)
        send(t, 2, 1)

    def relay_far(t):
        arrived(t, 2, 0)
        send(t, 2, 3)
        arrived(t, 2, 1)
        send(t, 2, 2)

    def near_rest(t, d):
        for q in ((1, 2, 3) if d == 1 else (2, 3)):
            arrived(t, d, q)

    def far_rest(t):
        arrived(t, 2, 2)
        arrived(t, 2, 3)

    send_own(WI)
    send_own(WO)
    send_own(GU)
    for offset in range(1, n):
        remote(sc_in, sc_all.at[n - offset - 1], sc_send.at[n - offset - 1], sc_recv.at[n - offset - 1], to_fs(offset))
    for k in (1, 2, 3):
        remote(ps_in, ps_all.at[k - 1], tp_send.at[2, k - 1], tp_recv.at[2, k - 1], {"tp": peers[k]})
    own_wi = pltpu.make_async_copy(wi_in, wi_all.at[0, 0], loc.at[0])
    own_wo = pltpu.make_async_copy(wo_in, wo_all.at[0, 0], loc.at[1])
    own_wi.start()
    own_wo.start()

    def normed_rows(values, gain):
        mean_sq = jnp.mean(values * values, axis=-1, keepdims=True)
        return (values * lax.rsqrt(mean_sq + eps) * gain).astype(bf16)

    stage[:, 0:halo, :] = jnp.zeros((n, halo, slab), bf16)

    @pl.loop(0, seq // 32)
    def _(i):
        rows = pl.ds(pl.multiple_of(i * 32, 32), 32)
        first[rows, :] = normed_rows(tok[rows, :].astype(f32), gains[0:1, :])

    def dot(a, b):
        return jnp.dot(a, b, preferred_element_type=f32)

    def gate_up(d, fresh):
        weights = slot(GU, d)
        cols = owner_cols(d)

        @pl.loop(0, weights.shape[1] // TILE)
        def _(j):
            at = pl.ds(pl.multiple_of(j * TILE, TILE), TILE)
            term = dot(first[:, cols], weights[:, at])
            if fresh:
                gacc[:, at] = term
            else:
                gacc[:, at] += term

    def activate(gate, upper, at):
        gate = gate * hs[0:1, at]
        upper = upper * hs[1:2, at]
        return (gate / (1.0 + jnp.exp(-gate)) * upper).astype(bf16)

    def down(d, top):
        weights = slot(DN, d)

        @pl.loop(0, slab // TILE)
        def _(j):
            at = pl.ds(pl.multiple_of(j * TILE, TILE), TILE)
            stage[d, top:top + seq, at] = dot(hidden[...], weights[:, at]).astype(bf16)

    gate_up(0, True)
    relay_near(WI)
    relay_near(WO)
    relay_near(GU)
    send_own(DN)
    relay_far(WI)
    relay_far(WO)
    for t in (WI, WO):
        near_rest(t, 1)
        near_rest(t, n - 1)
        far_rest(t)
    own_wi.wait()
    own_wo.wait()
    for k in (1, 2, 3):
        remote(wi_all.at[0], wi_all.at[k], tp_send.at[0, k - 1], tp_recv.at[0, k - 1], {"tp": peers[k]})
        remote(wo_all.at[0], wo_all.at[k], tp_send.at[1, k - 1], tp_recv.at[1, k - 1], {"tp": peers[k]})
    near_rest(GU, 1)
    gate_up(1, False)
    near_rest(GU, n - 1)
    gate_up(n - 1, False)
    relay_far(GU)
    relay_near(DN)
    far_rest(GU)
    gate_up(2, False)

    @pl.loop(0, units // TILE)
    def _(j):
        at = pl.ds(pl.multiple_of(j * TILE, TILE), TILE)
        up_at = pl.ds(pl.multiple_of(units + j * TILE, TILE), TILE)
        hidden[:, at] = activate(gacc[:, at], gacc[:, up_at], at)

    def scatter_one(d):
        down(d, halo)
        for k in (2, 3, 1):
            rows = pl.ds(pl.multiple_of(peers[k] * share, share), share + halo)
            remote(stage.at[d, rows, :], rs.at[d, k - 1], rs_send.at[d, k - 1], rs_recv.at[d, k - 1], {"tp": peers[k]})

    scatter_one(0)
    near_rest(DN, 1)
    scatter_one(1)
    near_rest(DN, n - 1)
    scatter_one(n - 1)
    relay_far(DN)
    for d in range(1, n):
        landed(sc_all.at[d - 1], sc_send.at[d - 1], sc_recv.at[d - 1])

    def scales(d):
        return sc_in if d == 0 else sc_all.at[d - 1]

    own_window = pl.ds(pl.multiple_of(me * share, share), share + halo)
    own_rows = pl.ds(pl.multiple_of(me * share, share), share)
    before = pl.ds(pl.multiple_of((me * share + seq - halo) % seq, halo), halo)

    def gather_one(d):
        total = stage[d, own_window, :].astype(f32)
        for k in (1, 2, 3):
            landed(rs.at[d, k - 1], rs_send.at[d, k - 1], rs_recv.at[d, k - 1])
            total = total + rs[d, k - 1].astype(f32)
        total = 0.5 * (total * scales(d)[0:1, :])
        cols = owner_cols(d)
        r1[0:halo, cols] = total[0:halo] + jnp.where(me > 0, tok[before, cols].astype(f32), 0.0)
        r1[halo:, cols] = total[halo:] + tok[own_rows, cols].astype(f32)

    gather_one(0)
    gather_one(1)
    gather_one(n - 1)
    far_rest(DN)
    scatter_one(2)
    for t in (0, 1, 2):
        for k in (1, 2, 3):
            where = (wi_all.at[k], wo_all.at[k], ps_all.at[k - 1])[t]
            landed(where, tp_send.at[t, k - 1], tp_recv.at[t, k - 1])
    gather_one(2)

    second[...] = normed_rows(r1[...], gains[1:2, :])
    for k in range(4):
        group = me if k == 0 else peers[k]
        total = dot(second[:, owner_cols(0)], wi_all[k, 0])
        for d in range(1, n):
            total = total + dot(second[:, owner_cols(d)], wi_all[k, d])
        values = (total * isc[pl.ds(group, 1), :]).astype(bf16).astype(f32)
        sum2 = values + pltpu.roll(values, 1, 0)
        sum4 = sum2 + pltpu.roll(sum2, 2, 0)
        sum8 = sum4 + pltpu.roll(sum4, 4, 0)
        sum16 = sum8 + pltpu.roll(sum8, 8, 0)
        summed = jnp.where(group == 0, sum2, jnp.where(group == 1, sum4, jnp.where(group == 2, sum8, sum16)))
        span = jnp.where(group == 0, 2, jnp.where(group == 1, 4, jnp.where(group == 2, 8, 16)))
        position = lax.broadcasted_iota(jnp.int32, (share, gc), 0) + me * share
        counts = jnp.minimum(position + 1, span).astype(f32)
        pooled = (summed[halo:] / counts - values[halo:]).astype(bf16)
        pscale = (ps_in if k == 0 else ps_all.at[k - 1])[0:1, :]
        pool[k] = (dot(pooled, pmap[group]) * pscale).astype(bf16)
    for d in range(n):
        cols = owner_cols(d)
        total = dot(pool[0], wo_all[0, d])
        for k in range(1, 4):
            total = total + dot(pool[k], wo_all[k, d])
        r2[:, cols] = r1[halo:, cols] + total * scales(d)[1:2, :]
    third[own_rows, :] = normed_rows(r2[...], gains[2:3, :])

    def rows_of(rank, count=1):
        return pl.ds(pl.multiple_of(rank * share, share), share * count)

    def gather_rows(ref, cols, s):
        mine = ref.at[rows_of(me), cols]
        remote(mine, mine, ag_send.at[s, 1], ag_recv.at[s, 1], {"tp": across})
        remote(mine, mine, ag_send.at[s, 0], ag_recv.at[s, 0], {"tp": mate})

    def forward_rows(ref, cols, s):
        theirs = ref.at[rows_of(across), cols]
        landed(theirs, ag_send.at[s, 1], ag_recv.at[s, 1])
        remote(theirs, theirs, ag_send.at[s, 2], ag_recv.at[s, 2], {"tp": mate})

    everything = slice(None)
    gather_rows(third, everything, n)
    landed(third.at[rows_of(mate), :], ag_send.at[n, 0], ag_recv.at[n, 0])

    def hidden_half(chip):
        rows = rows_of(2 * chip, 2)

        @pl.loop(0, units // TILE)
        def _(j):
            at = pl.ds(pl.multiple_of(j * TILE, TILE), TILE)
            up_at = pl.ds(pl.multiple_of(units + j * TILE, TILE), TILE)
            gate = upper = None
            for d in range(n):
                weights = slot(GU, d)
                left = third[rows, owner_cols(d)]
                g, u = dot(left, weights[:, at]), dot(left, weights[:, up_at])
                gate, upper = (g, u) if gate is None else (gate + g, upper + u)
            hidden[rows, at] = activate(gate, upper, at)

    for copy in started:
        copy.wait_send()
    started.clear()
    forward_rows(third, everything, n)
    hidden_half(me // 2)
    landed(third.at[rows_of(diag), :], ag_send.at[n, 2], ag_recv.at[n, 2])
    hidden_half(1 - me // 2)
    for d in range(n):
        down(d, 0)
        remote(stage.at[d, rows_of(diag), :], rs_a.at[d, 1], rs_send.at[n + d, 1], rs_recv.at[n + d, 1], {"tp": mate})
        remote(stage.at[d, rows_of(mate), :], rs_a.at[d, 0], rs_send.at[n + d, 0], rs_recv.at[n + d, 0], {"tp": mate})
    for d in range(n):
        landed(rs_a.at[d, 1], rs_send.at[n + d, 1], rs_recv.at[n + d, 1])
        s_b[d] = (stage[d, rows_of(across), :].astype(f32) + rs_a[d, 1].astype(f32)).astype(bf16)
        remote(s_b.at[d], rs_b.at[d], rs_send.at[n + d, 2], rs_recv.at[n + d, 2], {"tp": across})
    for d in range(n):
        landed(rs_a.at[d, 0], rs_send.at[n + d, 0], rs_recv.at[n + d, 0])
        landed(rs_b.at[d], rs_send.at[n + d, 2], rs_recv.at[n + d, 2])
        total = stage[d, rows_of(me), :].astype(f32) + rs_a[d, 0].astype(f32) + rs_b[d].astype(f32)
        cols = owner_cols(d)
        out[rows_of(me), cols] = (r2[:, cols] + 0.5 * (total * scales(d)[0:1, :])).astype(bf16)
        gather_rows(out, cols, d)
    for d in range(n):
        forward_rows(out, owner_cols(d), d)
    for d in range(n):
        landed(out.at[rows_of(mate), owner_cols(d)], ag_send.at[d, 0], ag_recv.at[d, 0])
        landed(out.at[rows_of(diag), owner_cols(d)], ag_send.at[d, 2], ag_recv.at[d, 2])
    for copy in started:
        copy.wait_send()


def fused_layer(
    tokens, norm_gains, gate_weight, up_weight, hidden_scales, down_weight, down_scale, mix_in, in_scale,
    pool_map, pool_scale, mix_out, out_scale,
):
    n = lax.axis_size("fs")
    seq, width = tokens.shape
    slab, units = gate_weight.shape
    groups, gc, _ = pool_map.shape
    share = seq // 4
    padded = share + widest
    rank = lax.axis_index("tp")
    gate_up_in = jnp.concatenate([gate_weight.astype(bf16), up_weight.astype(bf16)], axis=1)
    down_in = down_weight.astype(bf16)
    in_cols = lax.dynamic_slice_in_dim(mix_in, rank * gc, gc, 1).astype(bf16)
    out_rows = mix_out.astype(bf16)
    own_scales = jnp.concatenate([down_scale[None], out_scale[None], jnp.zeros((6, slab), f32)], axis=0)
    own_pool = jnp.broadcast_to(pool_scale[None], (8, gc))
    vmem = pl.BlockSpec(memory_space=pltpu.VMEM)
    dma = pltpu.SemaphoreType.DMA
    args = (
        tokens, norm_gains, gate_up_in, hidden_scales, down_in, in_cols, out_rows, in_scale.reshape(groups, gc),
        pool_map.astype(bf16), own_pool, own_scales,
    )
    return pl.pallas_call(
        functools.partial(layer_kernel, n),
        out_shape=jax.ShapeDtypeStruct((seq, width), bf16),
        in_specs=[vmem] * len(args),
        out_specs=vmem,
        scratch_shapes=[
            pltpu.VMEM((n - 1, slab, 2 * units), bf16),
            pltpu.VMEM((n - 1, units, slab), bf16),
            pltpu.VMEM((4, n, slab, gc), bf16),
            pltpu.VMEM((4, n, gc, slab), bf16),
            pltpu.VMEM((n - 1, 8, slab), f32),
            pltpu.VMEM((3, 8, gc), f32),
            pltpu.VMEM((seq, width), bf16),
            pltpu.VMEM((seq, 2 * units), f32),
            pltpu.VMEM((seq, units), bf16),
            pltpu.VMEM((n, seq + widest, slab), bf16),
            pltpu.VMEM((n, 3, padded, slab), bf16),
            pltpu.VMEM((padded, width), f32),
            pltpu.VMEM((padded, width), bf16),
            pltpu.VMEM((4, share, gc), bf16),
            pltpu.VMEM((share, width), f32),
            pltpu.VMEM((seq, width), bf16),
            pltpu.VMEM((n, 2, share, slab), bf16),
            pltpu.VMEM((n, share, slab), bf16),
            pltpu.VMEM((n, share, slab), bf16),
            dma((4, n - 1, QUARTERS)), dma((4, n - 1, QUARTERS)),
            dma((n - 1,)), dma((n - 1,)),
            dma((3, 3)), dma((3, 3)),
            dma((2 * n, 3)), dma((2 * n, 3)),
            dma((n + 1, 3)), dma((n + 1, 3)),
            dma((2,)),
        ],
        compiler_params=pltpu.CompilerParams(
            collective_id=0, has_side_effects=True, vmem_limit_bytes=60 * 1024 * 1024
        ),
    )(*args)


def solution(mesh):
    body = fused_layer if fits_kernel(mesh) else per_device
    return jax.shard_map(
        body,
        mesh=mesh,
        in_specs=(
            P(("rep", "fs"), None),
            P(),
            P("fs", "tp"),
            P("fs", "tp"),
            P(None, "tp"),
            P("tp", "fs"),
            P("fs"),
            P("fs", None),
            P(),
            P(),
            P("tp"),
            P("tp", "fs"),
            P("fs"),
        ),
        out_specs=P(("rep", "fs"), None),
        check_vma=False,
    )
```

```python
import functools

import jax
import jax.numpy as jnp
from jax import lax
from jax.experimental import pallas as pl
from jax.experimental.pallas import tpu as pltpu
from jax.sharding import PartitionSpec as P

eps = 1e-06
widest = 16


def normed(values, gain):
    mean_sq = jnp.mean(values * values, axis=-1, keepdims=True)
    return (values * lax.rsqrt(mean_sq + eps) * gain).astype(jnp.bfloat16)


def scatter_rows(term_fn, share):
    return lax.psum_scatter(
        term_fn(jnp.int32(0), lax.axis_size("tp") * share).astype(jnp.bfloat16),
        "tp",
        scatter_dimension=0,
        tiled=True,
    ).astype(jnp.float32)


def whole_rows(values):
    return lax.all_gather(values, "tp", axis=0, tiled=True)


def fetch_mixer(in_cols, mix_out):
    return (
        lax.all_gather(in_cols.astype(jnp.bfloat16), "fs", axis=0, tiled=True),
        lax.all_gather(mix_out.astype(jnp.bfloat16), "fs", axis=1, tiled=True),
    )


def hidden_units(rows_in, gate_full, up_full, hidden_scales):
    gate = jnp.dot(rows_in, gate_full, preferred_element_type=jnp.float32) * hidden_scales[0]
    upper = jnp.dot(rows_in, up_full, preferred_element_type=jnp.float32) * hidden_scales[1]
    return (jax.nn.silu(gate) * upper).astype(jnp.bfloat16)


def ffn_partial(normed_rows, gate_full, up_full, down_full, hidden_scales, share):

    def term_rows(row_start, row_count):
        hidden = hidden_units(normed_rows, gate_full, up_full, hidden_scales)
        return jnp.dot(hidden, down_full, preferred_element_type=jnp.float32)

    return scatter_rows(term_rows, share)


def per_device(
    tokens,
    norm_gains,
    gate_weight,
    up_weight,
    hidden_scales,
    down_weight,
    down_scale,
    mix_in,
    in_scale,
    pool_map,
    pool_scale,
    mix_out,
    out_scale,
):
    tp_width = lax.axis_size("tp")
    tp_rank = lax.axis_index("tp")
    seq_rows = tokens.shape[0]
    share = seq_rows // tp_width
    local_channels = mix_out.shape[0]
    group_width = pool_map.shape[1]
    needed = max(group_width, local_channels)
    first_channel = tp_rank * local_channels
    in_start = first_channel // group_width * group_width
    in_cols = lax.dynamic_slice_in_dim(mix_in, in_start, needed, 1)
    scale_cols = lax.dynamic_slice_in_dim(in_scale, in_start, needed, 0)
    down_cols, out_cols = (
        lax.all_gather(down_scale, "fs", axis=0, tiled=True),
        lax.all_gather(out_scale, "fs", axis=0, tiled=True),
    )
    gate_bf = gate_weight.astype(jnp.bfloat16)
    up_bf = up_weight.astype(jnp.bfloat16)
    down_bf = down_weight.astype(jnp.bfloat16)
    resid_all = tokens.astype(jnp.float32)
    first = normed(resid_all, norm_gains[0])
    gate_full, up_full, down_full = (
        lax.all_gather(gate_bf, "fs", axis=0, tiled=True),
        lax.all_gather(up_bf, "fs", axis=0, tiled=True),
        lax.all_gather(down_bf, "fs", axis=1, tiled=True),
    )
    ffn_one = ffn_partial(first, gate_full, up_full, down_full, hidden_scales, share)
    own_rows = lax.dynamic_slice_in_dim(resid_all, tp_rank * share, share, 0)
    resid_one = own_rows + 0.5 * (ffn_one * down_cols)
    second = whole_rows(normed(resid_one, norm_gains[1]))
    in_full, out_full = fetch_mixer(in_cols, mix_out)
    pool_in = (jnp.dot(second, in_full, preferred_element_type=jnp.float32) * scale_cols).astype(
        jnp.bfloat16
    )
    channel = in_start + jnp.arange(needed, dtype=jnp.int32)
    window = jnp.left_shift(jnp.int32(2), channel // group_width)
    position = jnp.arange(seq_rows, dtype=jnp.int32)[:, None]
    values = pool_in.astype(jnp.float32)
    summed = jnp.zeros_like(values)
    for offset in range(widest):
        shifted = jnp.pad(values, ((offset, 0), (0, 0)))[:seq_rows]
        summed = summed + jnp.where(offset < window, shifted, 0.0)
    counts = jnp.minimum(position + 1, window).astype(jnp.float32)
    pooled = (summed / counts - values).astype(jnp.bfloat16)
    map_bf = pool_map.astype(jnp.bfloat16)
    if local_channels < group_width:
        group_index = first_channel // group_width
        column_start = first_channel % group_width
        map_cols = lax.dynamic_slice(
            map_bf, (group_index, jnp.int32(0), column_start), (1, group_width, local_channels)
        )[0]
        grouped = jnp.dot(pooled, map_cols, preferred_element_type=jnp.float32)
    else:
        held_groups = local_channels // group_width
        maps_held = lax.dynamic_slice_in_dim(map_bf, first_channel // group_width, held_groups, 0)
        grouped = jnp.einsum(
            "tgc,gcd->tgd",
            pooled.reshape(seq_rows, held_groups, group_width),
            maps_held,
            preferred_element_type=jnp.float32,
        ).reshape(seq_rows, local_channels)
    pool_out = (grouped * pool_scale).astype(jnp.bfloat16)

    def mixer_rows(row_start, row_count):
        return jnp.dot(pool_out, out_full, preferred_element_type=jnp.float32)

    mixed = scatter_rows(mixer_rows, share)
    resid_two = resid_one + mixed * out_cols
    third = whole_rows(normed(resid_two, norm_gains[2]))
    ffn_two = ffn_partial(third, gate_full, up_full, down_full, hidden_scales, share)
    final_rows = (resid_two + 0.5 * (ffn_two * down_cols)).astype(jnp.bfloat16)
    return whole_rows(final_rows)


MESH = pl.DeviceIdType.MESH
QUARTERS = 4
TILE = 256
bf16 = jnp.bfloat16
f32 = jnp.float32


def fits_kernel(mesh):
    return mesh.shape["rep"] == 2 and mesh.shape["fs"] == 4 and mesh.shape["tp"] == 4


def layer_kernel(
    n, tok, gains, gate_hbm, up_hbm, hs, down_hbm, mix_in_hbm, mix_out_hbm, isc, pmap, pool_scale, down_scale, out_scale,
    out, gu_in, dn_in, wi_in, wo_in, wide_gate, wide_up, wide_down, wide_in, wide_out, sc_in, ps_in, gu_buf, dn_buf, wi_all, wo_all, sc_all, ps_all,
    first, gacc, hidden, stage, rs, r1, second, pool, r2, third, rs_a, s_b, rs_b,
    ring_send, ring_recv, sc_send, sc_recv, tp_send, tp_recv, rs_send, rs_recv, ag_send, ag_recv, loc,
):
    rep, fs, me = lax.axis_index("rep"), lax.axis_index("fs"), lax.axis_index("tp")
    width = tok.shape[1]
    seq = tok.shape[0]
    slab = width // n
    share = seq // 4
    halo = widest
    units = hs.shape[1]
    gc = pmap.shape[1]
    core = me % 2
    mate = me + 1 - 2 * core
    across = (me + 2) % 4
    diag = (mate + 2) % 4
    peers = {1: mate, 2: across, 3: diag}

    order = (
        fs,
        jnp.where(fs == 0, 1, fs - 1),
        jnp.where(fs == 0, 2, jnp.where(fs == 1, 2, jnp.where(fs == 2, 3, 1))),
        jnp.where(fs < 2, 3, 0),
    )

    def owner_cols(i):
        return pl.ds(pl.multiple_of(order[i] * slab, slab), slab)

    def to_fs(offset):
        return {"fs": (fs + offset + n) % n}

    columns_in = pl.ds(pl.multiple_of(me * gc, gc), gc)
    loads = [
        pltpu.make_async_copy(mix_in_hbm.at[:, columns_in], wide_in, loc.at[2]),
        pltpu.make_async_copy(mix_out_hbm, wide_out, loc.at[3]),
        pltpu.make_async_copy(gate_hbm, wide_gate, loc.at[4]),
        pltpu.make_async_copy(up_hbm, wide_up, loc.at[5]),
        pltpu.make_async_copy(down_hbm, wide_down, loc.at[6]),
    ]
    for load in loads:
        load.start()
    sc_in[...] = jnp.zeros_like(sc_in)
    sc_in[0:1, :] = down_scale[...]
    sc_in[1:2, :] = out_scale[...]
    ps_in[...] = jnp.broadcast_to(pool_scale[...], ps_in.shape)

    barrier = pltpu.get_barrier_semaphore()
    for offset in range(1, n):
        pl.semaphore_signal(barrier, inc=1, device_id=to_fs(offset), device_id_type=MESH)
    for k in (1, 2, 3):
        pl.semaphore_signal(barrier, inc=1, device_id={"tp": peers[k]}, device_id_type=MESH)
    pl.semaphore_signal(barrier, inc=1, device_id={"rep": 1 - rep}, device_id_type=MESH)

    WI, WO, GU, DN = range(4)

    def slot(t, i):
        if t == WI:
            return wi_in if i == 0 else wi_all.at[0, order[i]]
        if t == WO:
            return wo_in if i == 0 else wo_all.at[0, order[i]]
        if t == GU:
            return gu_in if i == 0 else gu_buf.at[order[i]]
        return dn_in if i == 0 else dn_buf.at[order[i]]

    def there(t):
        return (wi_all.at[0], wo_all.at[0], gu_buf, dn_buf)[t]

    def quarter(ref, at):
        rows = ref.shape[0] // QUARTERS
        return ref.at[pl.ds(pl.multiple_of(at * rows, rows), rows), :]

    started = []

    def start_if(cond, copy):
        if cond is None:
            copy.start()
        else:
            @pl.when(cond)
            def _():
                copy.start()
        started.append((cond, copy))

    def wait_sent():
        for cond, copy in started:
            if cond is None:
                copy.wait_send()
            else:
                @pl.when(cond)
                def _():
                    copy.wait_send()
        started.clear()

    UP, BACK, REP = range(3)

    def send(t, i, u, way):
        at = rep * 2 + u
        shard = order[i]
        dev = (to_fs(1), to_fs(-1), {"rep": 1 - rep})[way]
        cond = (fs < n - 1, fs > 0, None)[way]
        if i > 0 and way != REP:
            cond = cond & ((shard < fs) if way == UP else (shard > fs))
        start_if(cond, pltpu.make_async_remote_copy(
            src_ref=quarter(slot(t, i), at), dst_ref=quarter(there(t).at[shard], at),
            send_sem=ring_send.at[way, t, i, u], recv_sem=ring_recv.at[t, shard, at],
            device_id=dev, device_id_type=MESH,
        ))

    def arrived(t, i, at):
        here = quarter(slot(t, i), at)
        pltpu.make_async_remote_copy(
            src_ref=here, dst_ref=here, send_sem=ring_send.at[0, t, i, 0], recv_sem=ring_recv.at[t, order[i], at],
            device_id={"rep": 1 - rep}, device_id_type=MESH,
        ).wait_recv()

    def remote(src, dst, s_sem, r_sem, dev):
        start_if(None, pltpu.make_async_remote_copy(
            src_ref=src, dst_ref=dst, send_sem=s_sem, recv_sem=r_sem, device_id=dev, device_id_type=MESH
        ))

    def landed(dst, s_sem, r_sem):
        pltpu.make_async_remote_copy(
            src_ref=dst, dst_ref=dst, send_sem=s_sem, recv_sem=r_sem, device_id={"tp": mate}, device_id_type=MESH
        ).wait_recv()

    def send_own(t):
        for u in range(2):
            send(t, 0, u, UP)
            send(t, 0, u, BACK)

    def relay(t, i):
        for u in range(2):
            arrived(t, i, rep * 2 + u)
            send(t, i, u, UP)
            send(t, i, u, BACK)
            send(t, i, u, REP)

    def rest(t, i):
        for u in range(2):
            arrived(t, i, (1 - rep) * 2 + u)

    loads[0].wait()
    loads[1].wait()
    wi_in[...] = wide_in[...].astype(bf16)
    wo_in[...] = wide_out[...].astype(bf16)
    loads[2].wait()
    loads[3].wait()

    @pl.loop(0, slab // 32)
    def _(j):
        rows = pl.ds(pl.multiple_of(j * 32, 32), 32)
        gu_in[rows, 0:units] = wide_gate[rows, :].astype(bf16)
        gu_in[rows, units:] = wide_up[rows, :].astype(bf16)

    pl.semaphore_wait(barrier, n - 1 + 4)
    send_own(WI)
    send_own(WO)
    send_own(GU)
    loads[4].wait()

    @pl.loop(0, units // 32)
    def _(j):
        rows = pl.ds(pl.multiple_of(j * 32, 32), 32)
        dn_in[rows, :] = wide_down[rows, :].astype(bf16)

    for offset in range(1, n):
        remote(sc_in, sc_all.at[fs], sc_send.at[offset - 1], sc_recv.at[fs], to_fs(offset))
    for k in (1, 2, 3):
        remote(ps_in, ps_all.at[k - 1], tp_send.at[2, k - 1], tp_recv.at[2, k - 1], {"tp": peers[k]})
    own_wi = pltpu.make_async_copy(wi_in, wi_all.at[0, fs], loc.at[0])
    own_wo = pltpu.make_async_copy(wo_in, wo_all.at[0, fs], loc.at[1])
    own_wi.start()
    own_wo.start()

    def normed_rows(values, gain):
        mean_sq = jnp.mean(values * values, axis=-1, keepdims=True)
        return (values * lax.rsqrt(mean_sq + eps) * gain).astype(bf16)

    stage[:, 0:halo, :] = jnp.zeros((n, halo, slab), bf16)

    @pl.loop(0, seq // 32)
    def _(i):
        rows = pl.ds(pl.multiple_of(i * 32, 32), 32)
        first[rows, :] = normed_rows(tok[rows, :].astype(f32), gains[0:1, :])

    def dot(a, b):
        return jnp.dot(a, b, preferred_element_type=f32)

    def gate_up(d, fresh):
        weights = slot(GU, d)
        cols = owner_cols(d)

        @pl.loop(0, weights.shape[1] // TILE)
        def _(j):
            at = pl.ds(pl.multiple_of(j * TILE, TILE), TILE)
            term = dot(first[:, cols], weights[:, at])
            if fresh:
                gacc[:, at] = term
            else:
                gacc[:, at] += term

    def activate(gate, upper, at):
        gate = gate * hs[0:1, at]
        upper = upper * hs[1:2, at]
        return (gate / (1.0 + jnp.exp(-gate)) * upper).astype(bf16)

    def down(d, top):
        weights = slot(DN, d)

        @pl.loop(0, slab // TILE)
        def _(j):
            at = pl.ds(pl.multiple_of(j * TILE, TILE), TILE)
            stage[d, top:top + seq, at] = dot(hidden[...], weights[:, at]).astype(bf16)

    gate_up(0, True)
    for t in (WI, WO, GU):
        relay(t, 1)
    send_own(DN)
    for t in (WI, WO, GU):
        relay(t, 2)
    rest(GU, 1)
    gate_up(1, False)
    for t in (WI, WO, GU):
        relay(t, 3)
    rest(GU, 2)
    gate_up(2, False)
    for t in (WI, WO):
        for i in range(1, n):
            rest(t, i)
    own_wi.wait()
    own_wo.wait()
    for k in (1, 2, 3):
        remote(wi_all.at[0], wi_all.at[k], tp_send.at[0, k - 1], tp_recv.at[0, k - 1], {"tp": peers[k]})
        remote(wo_all.at[0], wo_all.at[k], tp_send.at[1, k - 1], tp_recv.at[1, k - 1], {"tp": peers[k]})
    relay(DN, 1)
    rest(GU, 3)
    gate_up(3, False)

    @pl.loop(0, units // TILE)
    def _(j):
        at = pl.ds(pl.multiple_of(j * TILE, TILE), TILE)
        up_at = pl.ds(pl.multiple_of(units + j * TILE, TILE), TILE)
        hidden[:, at] = activate(gacc[:, at], gacc[:, up_at], at)

    def scatter_one(d):
        down(d, halo)
        for k in (2, 3, 1):
            rows = pl.ds(pl.multiple_of(peers[k] * share, share), share + halo)
            remote(stage.at[d, rows, :], rs.at[d, k - 1], rs_send.at[d, k - 1], rs_recv.at[d, k - 1], {"tp": peers[k]})

    for i in range(1, n):
        landed(sc_all.at[order[i]], sc_send.at[0], sc_recv.at[order[i]])

    def scales(d):
        return sc_in if d == 0 else sc_all.at[order[d]]

    own_window = pl.ds(pl.multiple_of(me * share, share), share + halo)
    own_rows = pl.ds(pl.multiple_of(me * share, share), share)
    before = pl.ds(pl.multiple_of((me * share + seq - halo) % seq, halo), halo)

    def gather_one(d):
        total = stage[d, own_window, :].astype(f32)
        for k in (1, 2, 3):
            landed(rs.at[d, k - 1], rs_send.at[d, k - 1], rs_recv.at[d, k - 1])
            total = total + rs[d, k - 1].astype(f32)
        total = 0.5 * (total * scales(d)[0:1, :])
        cols = owner_cols(d)
        r1[0:halo, cols] = total[0:halo] + jnp.where(me > 0, tok[before, cols].astype(f32), 0.0)
        r1[halo:, cols] = total[halo:] + tok[own_rows, cols].astype(f32)

    scatter_one(0)
    relay(DN, 2)
    rest(DN, 1)
    scatter_one(1)
    gather_one(0)
    relay(DN, 3)
    rest(DN, 2)
    scatter_one(2)
    gather_one(1)
    rest(DN, 3)
    scatter_one(3)
    gather_one(2)
    for t in (0, 1, 2):
        for k in (1, 2, 3):
            where = (wi_all.at[k], wo_all.at[k], ps_all.at[k - 1])[t]
            landed(where, tp_send.at[t, k - 1], tp_recv.at[t, k - 1])
    gather_one(3)

    second[...] = normed_rows(r1[...], gains[1:2, :])
    for k in range(4):
        group = me if k == 0 else peers[k]
        total = dot(second[:, owner_cols(0)], wi_all[k, fs])
        for d in range(1, n):
            total = total + dot(second[:, owner_cols(d)], wi_all[k, order[d]])
        values = (total * isc[pl.ds(group, 1), :]).astype(bf16).astype(f32)
        sum2 = values + pltpu.roll(values, 1, 0)
        sum4 = sum2 + pltpu.roll(sum2, 2, 0)
        sum8 = sum4 + pltpu.roll(sum4, 4, 0)
        sum16 = sum8 + pltpu.roll(sum8, 8, 0)
        summed = jnp.where(group == 0, sum2, jnp.where(group == 1, sum4, jnp.where(group == 2, sum8, sum16)))
        span = jnp.where(group == 0, 2, jnp.where(group == 1, 4, jnp.where(group == 2, 8, 16)))
        position = lax.broadcasted_iota(jnp.int32, (share, gc), 0) + me * share
        counts = jnp.minimum(position + 1, span).astype(f32)
        pooled = (summed[halo:] / counts - values[halo:]).astype(bf16)
        pscale = (ps_in if k == 0 else ps_all.at[k - 1])[0:1, :]
        pool[k] = (dot(pooled, pmap[group].astype(bf16)) * pscale).astype(bf16)
    for d in range(n):
        cols = owner_cols(d)
        total = dot(pool[0], wo_all[0, order[d]])
        for k in range(1, 4):
            total = total + dot(pool[k], wo_all[k, order[d]])
        r2[:, cols] = r1[halo:, cols] + total * scales(d)[1:2, :]
    third[own_rows, :] = normed_rows(r2[...], gains[2:3, :])

    def rows_of(rank, count=1):
        return pl.ds(pl.multiple_of(rank * share, share), share * count)

    def gather_rows(ref, cols, s):
        mine = ref.at[rows_of(me), cols]
        remote(mine, mine, ag_send.at[s, 1], ag_recv.at[s, 1], {"tp": across})
        remote(mine, mine, ag_send.at[s, 0], ag_recv.at[s, 0], {"tp": mate})

    def forward_rows(ref, cols, s):
        theirs = ref.at[rows_of(across), cols]
        landed(theirs, ag_send.at[s, 1], ag_recv.at[s, 1])
        remote(theirs, theirs, ag_send.at[s, 2], ag_recv.at[s, 2], {"tp": mate})

    everything = slice(None)
    gather_rows(third, everything, n)
    landed(third.at[rows_of(mate), :], ag_send.at[n, 0], ag_recv.at[n, 0])

    def hidden_half(chip):
        rows = rows_of(2 * chip, 2)

        @pl.loop(0, units // TILE)
        def _(j):
            at = pl.ds(pl.multiple_of(j * TILE, TILE), TILE)
            up_at = pl.ds(pl.multiple_of(units + j * TILE, TILE), TILE)
            gate = upper = None
            for d in range(n):
                weights = slot(GU, d)
                left = third[rows, owner_cols(d)]
                g, u = dot(left, weights[:, at]), dot(left, weights[:, up_at])
                gate, upper = (g, u) if gate is None else (gate + g, upper + u)
            hidden[rows, at] = activate(gate, upper, at)

    wait_sent()
    forward_rows(third, everything, n)
    hidden_half(me // 2)
    landed(third.at[rows_of(diag), :], ag_send.at[n, 2], ag_recv.at[n, 2])
    hidden_half(1 - me // 2)
    for d in range(n):
        down(d, 0)
        remote(stage.at[d, rows_of(diag), :], rs_a.at[d, 1], rs_send.at[n + d, 1], rs_recv.at[n + d, 1], {"tp": mate})
        remote(stage.at[d, rows_of(mate), :], rs_a.at[d, 0], rs_send.at[n + d, 0], rs_recv.at[n + d, 0], {"tp": mate})
    for d in range(n):
        landed(rs_a.at[d, 1], rs_send.at[n + d, 1], rs_recv.at[n + d, 1])
        s_b[d] = (stage[d, rows_of(across), :].astype(f32) + rs_a[d, 1].astype(f32)).astype(bf16)
        remote(s_b.at[d], rs_b.at[d], rs_send.at[n + d, 2], rs_recv.at[n + d, 2], {"tp": across})
    for d in range(n):
        landed(rs_a.at[d, 0], rs_send.at[n + d, 0], rs_recv.at[n + d, 0])
        landed(rs_b.at[d], rs_send.at[n + d, 2], rs_recv.at[n + d, 2])
        total = stage[d, rows_of(me), :].astype(f32) + rs_a[d, 0].astype(f32) + rs_b[d].astype(f32)
        cols = owner_cols(d)
        out[rows_of(me), cols] = (r2[:, cols] + 0.5 * (total * scales(d)[0:1, :])).astype(bf16)
        gather_rows(out, cols, d)
    for d in range(n):
        forward_rows(out, owner_cols(d), d)
    for d in range(n):
        landed(out.at[rows_of(mate), owner_cols(d)], ag_send.at[d, 0], ag_recv.at[d, 0])
        landed(out.at[rows_of(diag), owner_cols(d)], ag_send.at[d, 2], ag_recv.at[d, 2])
    wait_sent()


def fused_layer(
    tokens, norm_gains, gate_weight, up_weight, hidden_scales, down_weight, down_scale, mix_in, in_scale,
    pool_map, pool_scale, mix_out, out_scale,
):
    n = lax.axis_size("fs")
    seq, width = tokens.shape
    slab, units = gate_weight.shape
    groups, gc, _ = pool_map.shape
    share = seq // 4
    padded = share + widest
    vmem = pl.BlockSpec(memory_space=pltpu.VMEM)
    dma = pltpu.SemaphoreType.DMA
    hbm = pl.BlockSpec(memory_space=pl.ANY)
    args = (
        (tokens, vmem), (norm_gains, vmem), (gate_weight, hbm), (up_weight, hbm), (hidden_scales, vmem),
        (down_weight, hbm), (mix_in, hbm), (mix_out, hbm), (in_scale.reshape(groups, gc), vmem), (pool_map, vmem),
        (pool_scale[None], vmem), (down_scale[None], vmem), (out_scale[None], vmem),
    )
    return pl.pallas_call(
        functools.partial(layer_kernel, n),
        out_shape=jax.ShapeDtypeStruct((seq, width), bf16),
        in_specs=[spec for _, spec in args],
        out_specs=vmem,
        scratch_shapes=[
            pltpu.VMEM((slab, 2 * units), bf16),
            pltpu.VMEM((units, slab), bf16),
            pltpu.VMEM((slab, gc), bf16),
            pltpu.VMEM((gc, slab), bf16),
            pltpu.VMEM((slab, units), f32),
            pltpu.VMEM((slab, units), f32),
            pltpu.VMEM((units, slab), f32),
            pltpu.VMEM((slab, gc), f32),
            pltpu.VMEM((gc, slab), f32),
            pltpu.VMEM((8, slab), f32),
            pltpu.VMEM((8, gc), f32),
            pltpu.VMEM((n, slab, 2 * units), bf16),
            pltpu.VMEM((n, units, slab), bf16),
            pltpu.VMEM((4, n, slab, gc), bf16),
            pltpu.VMEM((4, n, gc, slab), bf16),
            pltpu.VMEM((n, 8, slab), f32),
            pltpu.VMEM((3, 8, gc), f32),
            pltpu.VMEM((seq, width), bf16),
            pltpu.VMEM((seq, 2 * units), f32),
            pltpu.VMEM((seq, units), bf16),
            pltpu.VMEM((n, seq + widest, slab), bf16),
            pltpu.VMEM((n, 3, padded, slab), bf16),
            pltpu.VMEM((padded, width), f32),
            pltpu.VMEM((padded, width), bf16),
            pltpu.VMEM((4, share, gc), bf16),
            pltpu.VMEM((share, width), f32),
            pltpu.VMEM((seq, width), bf16),
            pltpu.VMEM((n, 2, share, slab), bf16),
            pltpu.VMEM((n, share, slab), bf16),
            pltpu.VMEM((n, share, slab), bf16),
            dma((3, 4, n, 2)), dma((4, n, QUARTERS)),
            dma((n - 1,)), dma((n,)),
            dma((3, 3)), dma((3, 3)),
            dma((2 * n, 3)), dma((2 * n, 3)),
            dma((n + 1, 3)), dma((n + 1, 3)),
            dma((7,)),
        ],
        compiler_params=pltpu.CompilerParams(
            collective_id=0, has_side_effects=True, vmem_limit_bytes=60 * 1024 * 1024
        ),
    )(*[value for value, _ in args])


def solution(mesh):
    body = fused_layer if fits_kernel(mesh) else per_device
    return jax.shard_map(
        body,
        mesh=mesh,
        in_specs=(
            P(("rep", "fs"), None),
            P(),
            P("fs", "tp"),
            P("fs", "tp"),
            P(None, "tp"),
            P("tp", "fs"),
            P("fs"),
            P("fs", None),
            P(),
            P(),
            P("tp"),
            P("tp", "fs"),
            P("fs"),
        ),
        out_specs=P(("rep", "fs"), None),
        check_vma=False,
    )
```

```python
import functools

import jax
import jax.numpy as jnp
from jax import lax
from jax.experimental import pallas as pl
from jax.experimental.pallas import tpu as pltpu
from jax.sharding import PartitionSpec as P

eps = 1e-06
widest = 16


def normed(values, gain):
    mean_sq = jnp.mean(values * values, axis=-1, keepdims=True)
    return (values * lax.rsqrt(mean_sq + eps) * gain).astype(jnp.bfloat16)


def scatter_rows(term_fn, share):
    return lax.psum_scatter(
        term_fn(jnp.int32(0), lax.axis_size("tp") * share).astype(jnp.bfloat16),
        "tp",
        scatter_dimension=0,
        tiled=True,
    ).astype(jnp.float32)


def whole_rows(values):
    return lax.all_gather(values, "tp", axis=0, tiled=True)


def fetch_mixer(in_cols, mix_out):
    return (
        lax.all_gather(in_cols.astype(jnp.bfloat16), "fs", axis=0, tiled=True),
        lax.all_gather(mix_out.astype(jnp.bfloat16), "fs", axis=1, tiled=True),
    )


def hidden_units(rows_in, gate_full, up_full, hidden_scales):
    gate = jnp.dot(rows_in, gate_full, preferred_element_type=jnp.float32) * hidden_scales[0]
    upper = jnp.dot(rows_in, up_full, preferred_element_type=jnp.float32) * hidden_scales[1]
    return (jax.nn.silu(gate) * upper).astype(jnp.bfloat16)


def ffn_partial(normed_rows, gate_full, up_full, down_full, hidden_scales, share):

    def term_rows(row_start, row_count):
        hidden = hidden_units(normed_rows, gate_full, up_full, hidden_scales)
        return jnp.dot(hidden, down_full, preferred_element_type=jnp.float32)

    return scatter_rows(term_rows, share)


def per_device(
    tokens,
    norm_gains,
    gate_weight,
    up_weight,
    hidden_scales,
    down_weight,
    down_scale,
    mix_in,
    in_scale,
    pool_map,
    pool_scale,
    mix_out,
    out_scale,
):
    tp_width = lax.axis_size("tp")
    tp_rank = lax.axis_index("tp")
    seq_rows = tokens.shape[0]
    share = seq_rows // tp_width
    local_channels = mix_out.shape[0]
    group_width = pool_map.shape[1]
    needed = max(group_width, local_channels)
    first_channel = tp_rank * local_channels
    in_start = first_channel // group_width * group_width
    in_cols = lax.dynamic_slice_in_dim(mix_in, in_start, needed, 1)
    scale_cols = lax.dynamic_slice_in_dim(in_scale, in_start, needed, 0)
    down_cols, out_cols = (
        lax.all_gather(down_scale, "fs", axis=0, tiled=True),
        lax.all_gather(out_scale, "fs", axis=0, tiled=True),
    )
    gate_bf = gate_weight.astype(jnp.bfloat16)
    up_bf = up_weight.astype(jnp.bfloat16)
    down_bf = down_weight.astype(jnp.bfloat16)
    resid_all = tokens.astype(jnp.float32)
    first = normed(resid_all, norm_gains[0])
    gate_full, up_full, down_full = (
        lax.all_gather(gate_bf, "fs", axis=0, tiled=True),
        lax.all_gather(up_bf, "fs", axis=0, tiled=True),
        lax.all_gather(down_bf, "fs", axis=1, tiled=True),
    )
    ffn_one = ffn_partial(first, gate_full, up_full, down_full, hidden_scales, share)
    own_rows = lax.dynamic_slice_in_dim(resid_all, tp_rank * share, share, 0)
    resid_one = own_rows + 0.5 * (ffn_one * down_cols)
    second = whole_rows(normed(resid_one, norm_gains[1]))
    in_full, out_full = fetch_mixer(in_cols, mix_out)
    pool_in = (jnp.dot(second, in_full, preferred_element_type=jnp.float32) * scale_cols).astype(
        jnp.bfloat16
    )
    channel = in_start + jnp.arange(needed, dtype=jnp.int32)
    window = jnp.left_shift(jnp.int32(2), channel // group_width)
    position = jnp.arange(seq_rows, dtype=jnp.int32)[:, None]
    values = pool_in.astype(jnp.float32)
    summed = jnp.zeros_like(values)
    for offset in range(widest):
        shifted = jnp.pad(values, ((offset, 0), (0, 0)))[:seq_rows]
        summed = summed + jnp.where(offset < window, shifted, 0.0)
    counts = jnp.minimum(position + 1, window).astype(jnp.float32)
    pooled = (summed / counts - values).astype(jnp.bfloat16)
    map_bf = pool_map.astype(jnp.bfloat16)
    if local_channels < group_width:
        group_index = first_channel // group_width
        column_start = first_channel % group_width
        map_cols = lax.dynamic_slice(
            map_bf, (group_index, jnp.int32(0), column_start), (1, group_width, local_channels)
        )[0]
        grouped = jnp.dot(pooled, map_cols, preferred_element_type=jnp.float32)
    else:
        held_groups = local_channels // group_width
        maps_held = lax.dynamic_slice_in_dim(map_bf, first_channel // group_width, held_groups, 0)
        grouped = jnp.einsum(
            "tgc,gcd->tgd",
            pooled.reshape(seq_rows, held_groups, group_width),
            maps_held,
            preferred_element_type=jnp.float32,
        ).reshape(seq_rows, local_channels)
    pool_out = (grouped * pool_scale).astype(jnp.bfloat16)

    def mixer_rows(row_start, row_count):
        return jnp.dot(pool_out, out_full, preferred_element_type=jnp.float32)

    mixed = scatter_rows(mixer_rows, share)
    resid_two = resid_one + mixed * out_cols
    third = whole_rows(normed(resid_two, norm_gains[2]))
    ffn_two = ffn_partial(third, gate_full, up_full, down_full, hidden_scales, share)
    final_rows = (resid_two + 0.5 * (ffn_two * down_cols)).astype(jnp.bfloat16)
    return whole_rows(final_rows)


MESH = pl.DeviceIdType.MESH
PARTS = (1, 1, 2, 4)
FIRST_PART = (0, 1, 2, 4, 8)
TILE = 256
bf16 = jnp.bfloat16
f32 = jnp.float32


def fits_kernel(mesh):
    return mesh.shape["rep"] == 2 and mesh.shape["fs"] == 4 and mesh.shape["tp"] == 4


def layer_kernel(
    n, tok, gains, gate_hbm, up_hbm, hs, down_hbm, mix_in_hbm, mix_out_hbm, isc, pmap, pool_scale, down_scale, out_scale,
    out, gu_in, dn_in, wi_in, wo_in, wide_gate, wide_up, wide_down, wide_in, wide_out, sc_in, ps_in, gu_buf, dn_buf, wi_all, wo_all, sc_all, ps_all,
    first, gacc, hidden, stage, rs, r1, second, pool, r2, third, rs_a, s_b, rs_b,
    ring_send, ring_recv, sc_send, sc_recv, tp_send, tp_recv, rs_send, rs_recv, ag_send, ag_recv, loc,
):
    rep, fs, me = lax.axis_index("rep"), lax.axis_index("fs"), lax.axis_index("tp")
    width = tok.shape[1]
    seq = tok.shape[0]
    slab = width // n
    share = seq // 4
    halo = widest
    units = hs.shape[1]
    gc = pmap.shape[1]
    core = me % 2
    mate = me + 1 - 2 * core
    across = (me + 2) % 4
    diag = (mate + 2) % 4
    peers = {1: mate, 2: across, 3: diag}

    order = (
        fs,
        jnp.where(fs == 0, 1, fs - 1),
        jnp.where(fs == 0, 2, jnp.where(fs == 1, 2, jnp.where(fs == 2, 3, 1))),
        jnp.where(fs < 2, 3, 0),
    )

    def owner_cols(i):
        return pl.ds(pl.multiple_of(order[i] * slab, slab), slab)

    def to_fs(offset):
        return {"fs": (fs + offset + n) % n}

    columns_in = pl.ds(pl.multiple_of(me * gc, gc), gc)
    half = slab // 2
    mine_half = pl.ds(pl.multiple_of(rep * half, half), half)
    other_half = pl.ds(pl.multiple_of((1 - rep) * half, half), half)
    loads = [
        pltpu.make_async_copy(mix_in_hbm.at[:, columns_in], wide_in, loc.at[2]),
        pltpu.make_async_copy(mix_out_hbm, wide_out, loc.at[3]),
        pltpu.make_async_copy(gate_hbm.at[mine_half, :], wide_gate.at[mine_half, :], loc.at[4]),
        pltpu.make_async_copy(up_hbm.at[mine_half, :], wide_up.at[mine_half, :], loc.at[5]),
        pltpu.make_async_copy(gate_hbm.at[other_half, :], wide_gate.at[other_half, :], loc.at[6]),
        pltpu.make_async_copy(up_hbm.at[other_half, :], wide_up.at[other_half, :], loc.at[7]),
        pltpu.make_async_copy(down_hbm, wide_down, loc.at[8]),
    ]
    for load in loads:
        load.start()
    barrier = pltpu.get_barrier_semaphore()
    for offset in range(1, n):
        pl.semaphore_signal(barrier, inc=1, device_id=to_fs(offset), device_id_type=MESH)
    for k in (1, 2, 3):
        pl.semaphore_signal(barrier, inc=1, device_id={"tp": peers[k]}, device_id_type=MESH)
    pl.semaphore_signal(barrier, inc=1, device_id={"rep": 1 - rep}, device_id_type=MESH)
    sc_in[...] = jnp.zeros_like(sc_in)
    sc_in[0:1, :] = down_scale[...]
    sc_in[1:2, :] = out_scale[...]
    ps_in[...] = jnp.broadcast_to(pool_scale[...], ps_in.shape)

    WI, WO, GU, DN = range(4)

    def slot(t, i):
        if t == WI:
            return wi_in if i == 0 else wi_all.at[0, order[i]]
        if t == WO:
            return wo_in if i == 0 else wo_all.at[0, order[i]]
        if t == GU:
            return gu_in if i == 0 else gu_buf.at[order[i]]
        return dn_in if i == 0 else dn_buf.at[order[i]]

    def there(t):
        return (wi_all.at[0], wo_all.at[0], gu_buf, dn_buf)[t]

    def part_of(ref, t, at):
        rows = ref.shape[0] // (2 * PARTS[t])
        return ref.at[pl.ds(pl.multiple_of(at * rows, rows), rows), :]

    started = []

    def start_if(cond, copy):
        if cond is None:
            copy.start()
        else:
            @pl.when(cond)
            def _():
                copy.start()
        started.append((cond, copy))

    def wait_sent():
        for cond, copy in started:
            if cond is None:
                copy.wait_send()
            else:
                @pl.when(cond)
                def _():
                    copy.wait_send()
        started.clear()

    UP, BACK, REP = range(3)

    def send(t, i, u, way):
        at = rep * PARTS[t] + u
        shard = order[i]
        dev = (to_fs(1), to_fs(-1), {"rep": 1 - rep})[way]
        cond = (fs < n - 1, fs > 0, None)[way]
        if i > 0 and way != REP:
            cond = cond & ((shard < fs) if way == UP else (shard > fs))
        start_if(cond, pltpu.make_async_remote_copy(
            src_ref=part_of(slot(t, i), t, at), dst_ref=part_of(there(t).at[shard], t, at),
            send_sem=ring_send.at[way, i, FIRST_PART[t] + u], recv_sem=ring_recv.at[shard, 2 * FIRST_PART[t] + at],
            device_id=dev, device_id_type=MESH,
        ))

    def arrived(t, i, at):
        here = part_of(slot(t, i), t, at)
        pltpu.make_async_remote_copy(
            src_ref=here, dst_ref=here, send_sem=ring_send.at[0, i, 0], recv_sem=ring_recv.at[order[i], 2 * FIRST_PART[t] + at],
            device_id={"rep": 1 - rep}, device_id_type=MESH,
        ).wait_recv()

    def remote(src, dst, s_sem, r_sem, dev):
        start_if(None, pltpu.make_async_remote_copy(
            src_ref=src, dst_ref=dst, send_sem=s_sem, recv_sem=r_sem, device_id=dev, device_id_type=MESH
        ))

    def landed(dst, s_sem, r_sem):
        pltpu.make_async_remote_copy(
            src_ref=dst, dst_ref=dst, send_sem=s_sem, recv_sem=r_sem, device_id={"tp": mate}, device_id_type=MESH
        ).wait_recv()

    def send_own(t):
        for u in range(PARTS[t]):
            send(t, 0, u, UP)
            send(t, 0, u, BACK)

    def relay(t, i):
        for u in range(PARTS[t]):
            arrived(t, i, rep * PARTS[t] + u)
            send(t, i, u, UP)
            send(t, i, u, BACK)
            send(t, i, u, REP)

    def rest(t, i):
        for u in range(PARTS[t]):
            arrived(t, i, (1 - rep) * PARTS[t] + u)

    loads[0].wait()
    loads[1].wait()
    wi_in[...] = wide_in[...].astype(bf16)
    wo_in[...] = wide_out[...].astype(bf16)
    def cast_gate_up(start, count):
        @pl.loop(0, count // 32)
        def _(j):
            rows = pl.ds(pl.multiple_of(start + j * 32, 32), 32)
            gu_in[rows, 0:units] = wide_gate[rows, :].astype(bf16)
            gu_in[rows, units:] = wide_up[rows, :].astype(bf16)

    pl.semaphore_wait(barrier, n - 1 + 4)
    send_own(WI)
    send_own(WO)
    loads[2].wait()
    loads[3].wait()
    for u in range(PARTS[GU]):
        cast_gate_up(rep * half + u * (half // PARTS[GU]), half // PARTS[GU])
        send(GU, 0, u, UP)
        send(GU, 0, u, BACK)

    def share_mixer(i):
        for t, held, own in ((0, wi_all, wi_in), (1, wo_all, wo_in)):
            src = own if i == 0 else held.at[0, order[i]]
            remote(src, held.at[2, order[i]], tp_send.at[t, i, 1], tp_recv.at[t, i, 1], {"tp": across})
            remote(src, held.at[1, order[i]], tp_send.at[t, i, 0], tp_recv.at[t, i, 0], {"tp": mate})

    def pass_mixer(i):
        for t, held in ((0, wi_all), (1, wo_all)):
            landed(held.at[2, order[i]], tp_send.at[t, i, 1], tp_recv.at[t, i, 1])
            remote(held.at[2, order[i]], held.at[3, order[i]], tp_send.at[t, i, 2], tp_recv.at[t, i, 2], {"tp": mate})

    share_mixer(0)
    loads[4].wait()
    loads[5].wait()
    cast_gate_up((1 - rep) * half, half)
    loads[6].wait()

    @pl.loop(0, units // 32)
    def _(j):
        rows = pl.ds(pl.multiple_of(j * 32, 32), 32)
        dn_in[rows, :] = wide_down[rows, :].astype(bf16)

    for offset in range(1, n):
        remote(sc_in, sc_all.at[fs], sc_send.at[offset - 1], sc_recv.at[fs], to_fs(offset))
    for k in (1, 2, 3):
        remote(ps_in, ps_all.at[k - 1], tp_send.at[2, 0, k - 1], tp_recv.at[2, 0, k - 1], {"tp": peers[k]})
    own_wi = pltpu.make_async_copy(wi_in, wi_all.at[0, fs], loc.at[0])
    own_wo = pltpu.make_async_copy(wo_in, wo_all.at[0, fs], loc.at[1])
    own_wi.start()
    own_wo.start()

    def normed_rows(values, gain):
        mean_sq = jnp.mean(values * values, axis=-1, keepdims=True)
        return (values * lax.rsqrt(mean_sq + eps) * gain).astype(bf16)

    stage[:, 0:halo, :] = jnp.zeros((n, halo, slab), bf16)

    @pl.loop(0, seq // 32)
    def _(i):
        rows = pl.ds(pl.multiple_of(i * 32, 32), 32)
        first[rows, :] = normed_rows(tok[rows, :].astype(f32), gains[0:1, :])

    def dot(a, b):
        return jnp.dot(a, b, preferred_element_type=f32)

    def gate_up(d, fresh):
        weights = slot(GU, d)
        cols = owner_cols(d)

        @pl.loop(0, weights.shape[1] // TILE)
        def _(j):
            at = pl.ds(pl.multiple_of(j * TILE, TILE), TILE)
            term = dot(first[:, cols], weights[:, at])
            if fresh:
                gacc[:, at] = term
            else:
                gacc[:, at] += term

    def activate(gate, upper, at):
        gate = gate * hs[0:1, at]
        upper = upper * hs[1:2, at]
        return (gate / (1.0 + jnp.exp(-gate)) * upper).astype(bf16)

    def down(d, top):
        weights = slot(DN, d)

        @pl.loop(0, slab // TILE)
        def _(j):
            at = pl.ds(pl.multiple_of(j * TILE, TILE), TILE)
            stage[d, top:top + seq, at] = dot(hidden[...], weights[:, at]).astype(bf16)

    gate_up(0, True)
    for t in (WI, WO, GU):
        relay(t, 1)
    send_own(DN)
    for t in (WI, WO, GU):
        relay(t, 2)
    rest(WI, 1)
    rest(WO, 1)
    share_mixer(1)
    rest(GU, 1)
    gate_up(1, False)
    for t in (WI, WO, GU):
        relay(t, 3)
    pass_mixer(0)
    rest(WI, 2)
    rest(WO, 2)
    share_mixer(2)
    rest(GU, 2)
    gate_up(2, False)
    rest(WI, 3)
    rest(WO, 3)
    share_mixer(3)
    own_wi.wait()
    own_wo.wait()
    pass_mixer(1)
    relay(DN, 1)
    rest(GU, 3)
    gate_up(3, False)

    @pl.loop(0, units // TILE)
    def _(j):
        at = pl.ds(pl.multiple_of(j * TILE, TILE), TILE)
        up_at = pl.ds(pl.multiple_of(units + j * TILE, TILE), TILE)
        hidden[:, at] = activate(gacc[:, at], gacc[:, up_at], at)

    def scatter_one(d):
        down(d, halo)
        for k in (2, 3, 1):
            rows = pl.ds(pl.multiple_of(peers[k] * share, share), share + halo)
            remote(stage.at[d, rows, :], rs.at[d, k - 1], rs_send.at[d, k - 1], rs_recv.at[d, k - 1], {"tp": peers[k]})

    for i in range(1, n):
        landed(sc_all.at[order[i]], sc_send.at[0], sc_recv.at[order[i]])

    def scales(d):
        return sc_in if d == 0 else sc_all.at[order[d]]

    own_window = pl.ds(pl.multiple_of(me * share, share), share + halo)
    own_rows = pl.ds(pl.multiple_of(me * share, share), share)
    before = pl.ds(pl.multiple_of((me * share + seq - halo) % seq, halo), halo)

    def gather_one(d):
        total = stage[d, own_window, :].astype(f32)
        for k in (1, 2, 3):
            landed(rs.at[d, k - 1], rs_send.at[d, k - 1], rs_recv.at[d, k - 1])
            total = total + rs[d, k - 1].astype(f32)
        total = 0.5 * (total * scales(d)[0:1, :])
        cols = owner_cols(d)
        r1[0:halo, cols] = total[0:halo] + jnp.where(me > 0, tok[before, cols].astype(f32), 0.0)
        r1[halo:, cols] = total[halo:] + tok[own_rows, cols].astype(f32)

    scatter_one(0)
    relay(DN, 2)
    pass_mixer(2)
    rest(DN, 1)
    scatter_one(1)
    gather_one(0)
    relay(DN, 3)
    pass_mixer(3)
    rest(DN, 2)
    scatter_one(2)
    gather_one(1)
    rest(DN, 3)
    scatter_one(3)
    gather_one(2)
    for k in (1, 2, 3):
        landed(ps_all.at[k - 1], tp_send.at[2, 0, k - 1], tp_recv.at[2, 0, k - 1])
    for i in range(n):
        for t, held in ((0, wi_all), (1, wo_all)):
            landed(held.at[1, order[i]], tp_send.at[t, i, 0], tp_recv.at[t, i, 0])
            landed(held.at[3, order[i]], tp_send.at[t, i, 2], tp_recv.at[t, i, 2])
    gather_one(3)

    second[...] = normed_rows(r1[...], gains[1:2, :])
    for k in range(4):
        group = me if k == 0 else peers[k]
        total = dot(second[:, owner_cols(0)], wi_all[k, fs])
        for d in range(1, n):
            total = total + dot(second[:, owner_cols(d)], wi_all[k, order[d]])
        values = (total * isc[pl.ds(group, 1), :]).astype(bf16).astype(f32)
        sum2 = values + pltpu.roll(values, 1, 0)
        sum4 = sum2 + pltpu.roll(sum2, 2, 0)
        sum8 = sum4 + pltpu.roll(sum4, 4, 0)
        sum16 = sum8 + pltpu.roll(sum8, 8, 0)
        summed = jnp.where(group == 0, sum2, jnp.where(group == 1, sum4, jnp.where(group == 2, sum8, sum16)))
        span = jnp.where(group == 0, 2, jnp.where(group == 1, 4, jnp.where(group == 2, 8, 16)))
        position = lax.broadcasted_iota(jnp.int32, (share, gc), 0) + me * share
        counts = jnp.minimum(position + 1, span).astype(f32)
        pooled = (summed[halo:] / counts - values[halo:]).astype(bf16)
        pscale = (ps_in if k == 0 else ps_all.at[k - 1])[0:1, :]
        pool[k] = (dot(pooled, pmap[group].astype(bf16)) * pscale).astype(bf16)
    for d in range(n):
        cols = owner_cols(d)
        total = dot(pool[0], wo_all[0, order[d]])
        for k in range(1, 4):
            total = total + dot(pool[k], wo_all[k, order[d]])
        r2[:, cols] = r1[halo:, cols] + total * scales(d)[1:2, :]
    third[own_rows, :] = normed_rows(r2[...], gains[2:3, :])

    def rows_of(rank, count=1):
        return pl.ds(pl.multiple_of(rank * share, share), share * count)

    def gather_rows(ref, cols, s):
        mine = ref.at[rows_of(me), cols]
        remote(mine, mine, ag_send.at[s, 1], ag_recv.at[s, 1], {"tp": across})
        remote(mine, mine, ag_send.at[s, 0], ag_recv.at[s, 0], {"tp": mate})

    def forward_rows(ref, cols, s):
        theirs = ref.at[rows_of(across), cols]
        landed(theirs, ag_send.at[s, 1], ag_recv.at[s, 1])
        remote(theirs, theirs, ag_send.at[s, 2], ag_recv.at[s, 2], {"tp": mate})

    everything = slice(None)
    gather_rows(third, everything, n)
    landed(third.at[rows_of(mate), :], ag_send.at[n, 0], ag_recv.at[n, 0])

    def hidden_half(chip):
        rows = rows_of(2 * chip, 2)

        @pl.loop(0, units // TILE)
        def _(j):
            at = pl.ds(pl.multiple_of(j * TILE, TILE), TILE)
            up_at = pl.ds(pl.multiple_of(units + j * TILE, TILE), TILE)
            gate = upper = None
            for d in range(n):
                weights = slot(GU, d)
                left = third[rows, owner_cols(d)]
                g, u = dot(left, weights[:, at]), dot(left, weights[:, up_at])
                gate, upper = (g, u) if gate is None else (gate + g, upper + u)
            hidden[rows, at] = activate(gate, upper, at)

    wait_sent()
    forward_rows(third, everything, n)
    hidden_half(me // 2)
    landed(third.at[rows_of(diag), :], ag_send.at[n, 2], ag_recv.at[n, 2])
    hidden_half(1 - me // 2)
    for d in range(n):
        down(d, 0)
        remote(stage.at[d, rows_of(diag), :], rs_a.at[d, 1], rs_send.at[n + d, 1], rs_recv.at[n + d, 1], {"tp": mate})
        remote(stage.at[d, rows_of(mate), :], rs_a.at[d, 0], rs_send.at[n + d, 0], rs_recv.at[n + d, 0], {"tp": mate})
    for d in range(n):
        landed(rs_a.at[d, 1], rs_send.at[n + d, 1], rs_recv.at[n + d, 1])
        s_b[d] = (stage[d, rows_of(across), :].astype(f32) + rs_a[d, 1].astype(f32)).astype(bf16)
        remote(s_b.at[d], rs_b.at[d], rs_send.at[n + d, 2], rs_recv.at[n + d, 2], {"tp": across})
    for d in range(n):
        landed(rs_a.at[d, 0], rs_send.at[n + d, 0], rs_recv.at[n + d, 0])
        landed(rs_b.at[d], rs_send.at[n + d, 2], rs_recv.at[n + d, 2])
        total = stage[d, rows_of(me), :].astype(f32) + rs_a[d, 0].astype(f32) + rs_b[d].astype(f32)
        cols = owner_cols(d)
        out[rows_of(me), cols] = (r2[:, cols] + 0.5 * (total * scales(d)[0:1, :])).astype(bf16)
        gather_rows(out, cols, d)
    for d in range(n):
        forward_rows(out, owner_cols(d), d)
    for d in range(n):
        landed(out.at[rows_of(mate), owner_cols(d)], ag_send.at[d, 0], ag_recv.at[d, 0])
        landed(out.at[rows_of(diag), owner_cols(d)], ag_send.at[d, 2], ag_recv.at[d, 2])
    wait_sent()


def fused_layer(
    tokens, norm_gains, gate_weight, up_weight, hidden_scales, down_weight, down_scale, mix_in, in_scale,
    pool_map, pool_scale, mix_out, out_scale,
):
    n = lax.axis_size("fs")
    seq, width = tokens.shape
    slab, units = gate_weight.shape
    groups, gc, _ = pool_map.shape
    share = seq // 4
    padded = share + widest
    vmem = pl.BlockSpec(memory_space=pltpu.VMEM)
    dma = pltpu.SemaphoreType.DMA
    hbm = pl.BlockSpec(memory_space=pl.ANY)
    args = (
        (tokens, vmem), (norm_gains, vmem), (gate_weight, hbm), (up_weight, hbm), (hidden_scales, vmem),
        (down_weight, hbm), (mix_in, hbm), (mix_out, hbm), (in_scale.reshape(groups, gc), vmem), (pool_map, vmem),
        (pool_scale[None], vmem), (down_scale[None], vmem), (out_scale[None], vmem),
    )
    return pl.pallas_call(
        functools.partial(layer_kernel, n),
        out_shape=jax.ShapeDtypeStruct((seq, width), bf16),
        in_specs=[spec for _, spec in args],
        out_specs=vmem,
        scratch_shapes=[
            pltpu.VMEM((slab, 2 * units), bf16),
            pltpu.VMEM((units, slab), bf16),
            pltpu.VMEM((slab, gc), bf16),
            pltpu.VMEM((gc, slab), bf16),
            pltpu.VMEM((slab, units), f32),
            pltpu.VMEM((slab, units), f32),
            pltpu.VMEM((units, slab), f32),
            pltpu.VMEM((slab, gc), f32),
            pltpu.VMEM((gc, slab), f32),
            pltpu.VMEM((8, slab), f32),
            pltpu.VMEM((8, gc), f32),
            pltpu.VMEM((n, slab, 2 * units), bf16),
            pltpu.VMEM((n, units, slab), bf16),
            pltpu.VMEM((4, n, slab, gc), bf16),
            pltpu.VMEM((4, n, gc, slab), bf16),
            pltpu.VMEM((n, 8, slab), f32),
            pltpu.VMEM((3, 8, gc), f32),
            pltpu.VMEM((seq, width), bf16),
            pltpu.VMEM((seq, 2 * units), f32),
            pltpu.VMEM((seq, units), bf16),
            pltpu.VMEM((n, seq + widest, slab), bf16),
            pltpu.VMEM((n, 3, padded, slab), bf16),
            pltpu.VMEM((padded, width), f32),
            pltpu.VMEM((padded, width), bf16),
            pltpu.VMEM((4, share, gc), bf16),
            pltpu.VMEM((share, width), f32),
            pltpu.VMEM((seq, width), bf16),
            pltpu.VMEM((n, 2, share, slab), bf16),
            pltpu.VMEM((n, share, slab), bf16),
            pltpu.VMEM((n, share, slab), bf16),
            dma((3, n, FIRST_PART[-1])), dma((n, 2 * FIRST_PART[-1])),
            dma((n - 1,)), dma((n,)),
            dma((3, n, 3)), dma((3, n, 3)),
            dma((2 * n, 3)), dma((2 * n, 3)),
            dma((n + 1, 3)), dma((n + 1, 3)),
            dma((9,)),
        ],
        compiler_params=pltpu.CompilerParams(
            collective_id=0, has_side_effects=True, vmem_limit_bytes=60 * 1024 * 1024
        ),
    )(*[value for value, _ in args])


def solution(mesh):
    body = fused_layer if fits_kernel(mesh) else per_device
    return jax.shard_map(
        body,
        mesh=mesh,
        in_specs=(
            P(("rep", "fs"), None),
            P(),
            P("fs", "tp"),
            P("fs", "tp"),
            P(None, "tp"),
            P("tp", "fs"),
            P("fs"),
            P("fs", None),
            P(),
            P(),
            P("tp"),
            P("tp", "fs"),
            P("fs"),
        ),
        out_specs=P(("rep", "fs"), None),
        check_vma=False,
    )
```
